32 devices in a mesh: sp: 16 (over z, y, x), tp: 2 (over core).
Axes of the slice: x: 2, y: 2, z: 4, core: 2. Of those that a mesh axis runs over, the one named last changes fastest.
Arguments:
- block_input: bfloat16 [4096, 2048], P('sp'), may hold values from -6 to 6
- queries: bfloat16 [4096, 256], P('sp', 'tp'), may hold values from -13 to 13
- keys: bfloat16 [4096, 256], P('sp', 'tp'), may hold values from -13 to 13
- values: bfloat16 [4096, 512], P('sp', 'tp'), may hold values from -6 to 6
- in_gate: float32 [2, 4096], P('tp', 'sp'), may hold values from -110 to 100
- log_forget: float32 [2, 4096], P('tp', 'sp'), may hold values from -0.08 to 0
- grad_out: bfloat16 [4096, 512], P('sp', 'tp'), may hold values from -6 to 6
Outputs:
- grad_queries: bfloat16 [4096, 256], P('sp', 'tp')
- grad_keys: bfloat16 [4096, 256], P('sp', 'tp')
- grad_values: bfloat16 [4096, 512], P('sp', 'tp')
- grad_in_gate: float32 [2, 4096], P('tp', 'sp')
- grad_log_forget: float32 [2, 4096], P('tp', 'sp')
- grad_query_weight: float32 [2048, 256], P('sp', 'tp')
The draws below stay inside these ranges and needn't reach their ends.
All inputs are finite; a program needn't handle non-finite values.
Results may differ from the reference program's by a relative error of at most 0.012.
The reference program's roundings to bfloat16 on the way count: a program that leaves them out, or rounds other values in their place, can miss the bound.
Values sent between devices are 32-bit elements.
A program may use at most 64 MiB of HBM per device.

```python
import jax
import jax.numpy as jnp
from jax import lax

D = 2048
HEADS = 2
DK = 128
DV = 256
TOK_DEV = 256
TOKENS = 4096
N_SP = 16


def shared_direction(key):
    direction = jax.random.normal(jax.random.fold_in(key, 101), (HEADS, DK), jnp.float32)
    direction = direction / jnp.sqrt(jnp.sum(direction * direction, axis=1, keepdims=True))
    return direction * jnp.sqrt(4.0 * jnp.sqrt(1.0 * DK))


def head_entries(key, stream):
    jitter = jnp.clip(jax.random.normal(jax.random.fold_in(key, stream), (TOKENS, HEADS, DK), jnp.float32), -5.0, 5.0)
    entries = jitter + shared_direction(key)[None]
    return entries.reshape(TOKENS, HEADS * DK).astype(jnp.bfloat16)


def draw_queries(key, part):
    return head_entries(key, 1)


def draw_keys(key, part):
    return head_entries(key, 2)


def draw_values(key, part):
    entries = jnp.clip(jax.random.normal(jax.random.fold_in(key, 3), (TOKENS, HEADS * DV), jnp.float32), -6.0, 6.0)
    return entries.astype(jnp.bfloat16)


def draw_in_gate(key, part):
    blocks = TOKENS // TOK_DEV
    spread = jax.random.uniform(jax.random.fold_in(key, 11), (HEADS, TOKENS), jnp.float32, -3.0, 3.0)
    offset = jax.random.uniform(jax.random.fold_in(key, 12), (HEADS, blocks), jnp.float32, -2.0, 2.0)
    gate_pre = spread + jnp.repeat(offset, TOK_DEV, axis=1)
    return gate_pre


def draw_log_forget(key, part):
    blocks = TOKENS // TOK_DEV
    ranking = jax.random.permutation(jax.random.fold_in(key, 21), HEADS)
    quick = ranking < HEADS // 2
    slow_rate = 1.5 / TOKENS
    base_rate = jnp.where(quick, 0.02, slow_rate).astype(jnp.float32)
    by_block = jnp.exp(jax.random.uniform(jax.random.fold_in(key, 22), (HEADS, blocks), jnp.float32, -0.6931, 0.6931))
    by_step = jnp.exp(jax.random.uniform(jax.random.fold_in(key, 23), (HEADS, TOKENS), jnp.float32, -0.6931, 0.6931))
    return -(base_rate[:, None] * jnp.repeat(by_block, TOK_DEV, axis=1) * by_step)


def block_scale(own_key, extent, split, least, high):
    def one(axis_at, blocks):
        steps = jax.random.uniform(jax.random.fold_in(jax.random.fold_in(own_key, 6), axis_at), (blocks,), jnp.float32, least / len(split), high / len(split))
        return jnp.repeat(jnp.exp(steps), extent[axis_at] // blocks).reshape((-1,) + (1,) * (len(extent) - axis_at - 1))

    level = one(*split[0])
    for cut in split[1:]:
        level = level * one(*cut)
    return level


def bell_draw(own_key, extent, scale, reach, pieces=(), held_as=jnp.bfloat16):
    array = scale * jax.random.normal(own_key, extent, jnp.float32)
    if pieces:
        array = array * block_scale(own_key, extent, pieces, -0.22, 0.18)
    return jnp.clip(array, -reach, reach).astype(held_as)


def setup_inputs(seed: int = 0) -> dict:
    seeds = jax.random.split(jax.random.key(seed), 8)
    return {
        "block_input": bell_draw(seeds[0], (TOKENS, D), 1.0, 6.0, ((0, 16),)),
        "queries": draw_queries(jax.random.fold_in(seeds[7], 71), 0),
        "keys": draw_keys(jax.random.fold_in(seeds[7], 71), 0),
        "values": draw_values(jax.random.fold_in(seeds[7], 71), 0),
        "in_gate": draw_in_gate(jax.random.fold_in(seeds[7], 71), 0),
        "log_forget": draw_log_forget(jax.random.fold_in(seeds[7], 71), 0),
        "grad_out": bell_draw(seeds[6], (TOKENS, HEADS * DV), 1.0, 6.0, ((0, 16), (1, 2))),
    }


VERY_LOW = -1e+30
EXACT_MODE = lax.Precision.HIGHEST

def rounded(matrix):
    return lax.optimization_barrier(matrix.astype(jnp.bfloat16)).astype(jnp.float32)

def gate_sums(gate_row, forget_row):
    forget_sum = jnp.cumsum(forget_row, axis=1)
    block_total = forget_sum[:, -1]
    log_tail = block_total[:, None] - forget_sum + gate_row
    seg_max = lax.optimization_barrier(jnp.max(log_tail, axis=1))
    return (forget_sum, block_total, log_tail, seg_max)

def forward_summary(key_rows, row_values, gate_row, forget_row):
    scale_of_keys = key_rows.shape[-1] ** (-0.5)
    forget_sum, block_total, log_tail, seg_max = gate_sums(gate_row, forget_row)
    factor = jnp.exp(log_tail - seg_max[:, None])
    weighted_terms = rounded(key_rows.astype(jnp.float32) * factor.T[:, :, None])
    segment_matrix = scale_of_keys * jnp.einsum('uae,uap->aep', weighted_terms, row_values.astype(jnp.float32), precision=EXACT_MODE)
    seg_vec = scale_of_keys * lax.optimization_barrier(jnp.sum(weighted_terms, axis=0))
    return (block_total, seg_max, segment_matrix, seg_vec)

def join_forward(earlier, latter):
    earlier_sum, earlier_max, earlier_mat, earlier_vec = earlier
    latter_sum, latter_max, latter_mat, latter_vec = latter
    new_max = jnp.maximum(latter_sum + earlier_max, latter_max)
    keep_factor = jnp.exp(latter_sum + earlier_max - new_max)
    fresh_factor = jnp.exp(latter_max - new_max)
    return (earlier_sum + latter_sum, new_max, keep_factor[:, None, None] * earlier_mat + fresh_factor[:, None, None] * latter_mat, keep_factor[:, None] * earlier_vec + fresh_factor[:, None] * latter_vec)

def local_pass(row_queries, key_rows, row_values, grad_rows, gate_row, forget_row, enter_max, enter_mat, incoming_vector, outgoing_matrix, outgoing_vector):
    scale_of_keys = key_rows.shape[-1] ** (-0.5)
    length = row_queries.shape[0]
    forget_sum, block_total, log_tail, seg_max = gate_sums(gate_row, forget_row)
    broad_query = row_queries.astype(jnp.float32)
    broad_key = key_rows.astype(jnp.float32)
    broad_value = row_values.astype(jnp.float32)
    grad_wide = grad_rows.astype(jnp.float32)
    row_index = lax.broadcasted_iota(jnp.int32, (length, length), 0)
    col_index = lax.broadcasted_iota(jnp.int32, (length, length), 1)
    log_intra = jnp.where((col_index <= row_index)[None], forget_sum[:, :, None] - forget_sum[:, None, :] + gate_row[:, None, :], -jnp.inf)
    intra_max = lax.optimization_barrier(jnp.max(log_intra, axis=2))
    log_inter = forget_sum + enter_max[:, None]
    row_max = jnp.maximum(log_inter, intra_max)
    inter_weight = jnp.exp(log_inter - row_max)
    intra_weight = jnp.exp(log_intra - row_max[:, :, None])
    column_between = inter_weight.T[:, :, None]
    scores = scale_of_keys * jnp.einsum('thk,shk->hts', broad_query, broad_key, precision=EXACT_MODE)
    weighted_scores = intra_weight * scores
    lowered_score = rounded(weighted_scores)
    incoming_lowered = rounded(enter_mat)
    ratio_top = column_between * jnp.einsum('rpn,pns->rps', broad_query, incoming_lowered, precision=EXACT_MODE) + jnp.einsum('ynr,ryp->nyp', lowered_score, broad_value, precision=EXACT_MODE)
    denominator = inter_weight * jnp.einsum('thk,hk->ht', broad_query, incoming_vector, precision=EXACT_MODE) + lax.optimization_barrier(jnp.sum(weighted_scores, axis=2))
    floor_scale = jnp.sqrt(denominator * denominator + jnp.exp(-2.0 * row_max))
    lowered_delta = rounded(grad_wide / floor_scale.T[:, :, None])
    small_offset = -lax.optimization_barrier(jnp.sum(grad_wide * ratio_top, axis=2)).T * denominator / floor_scale ** 3
    errors = jnp.einsum('thv,shv->hts', lowered_delta, broad_value, precision=EXACT_MODE) + small_offset[:, :, None]
    backward_lowered = rounded(intra_weight * errors)
    query_gradient = scale_of_keys * jnp.einsum('flu,ufn->lfn', backward_lowered, broad_key, precision=EXACT_MODE) + column_between * (jnp.einsum('ojz,jlz->ojl', lowered_delta, incoming_lowered, precision=EXACT_MODE) + small_offset.T[:, :, None] * incoming_vector[None])
    leave_max = jnp.maximum(block_total + enter_max, seg_max)
    back_decay = block_total + enter_max - leave_max
    query_backward = rounded(broad_query * column_between)
    backward_matrix = jnp.einsum('url,urg->rlg', query_backward, lowered_delta, precision=EXACT_MODE)
    back_vec = jnp.einsum('ht,thk->hk', small_offset * inter_weight, broad_query, precision=EXACT_MODE)
    column_decay = jnp.exp(log_tail - leave_max[:, None]).T[:, :, None]
    key_gradient = scale_of_keys * jnp.einsum('cov,ocx->vcx', backward_lowered, broad_query, precision=EXACT_MODE) + scale_of_keys * column_decay * (jnp.einsum('rxi,xei->rxe', broad_value, outgoing_matrix, precision=EXACT_MODE) + outgoing_vector[None])
    value_gradient = jnp.einsum('zrf,rzp->fzp', lowered_score, lowered_delta, precision=EXACT_MODE) + scale_of_keys * column_decay * jnp.einsum('brz,rzf->brf', broad_key, outgoing_matrix, precision=EXACT_MODE)
    grad_gate = lax.optimization_barrier(jnp.sum(broad_key * key_gradient, axis=2)).T
    forget_part = lax.optimization_barrier(jnp.sum(broad_query * query_gradient, axis=2)).T - grad_gate
    inside = jnp.cumsum(forget_part, axis=1)
    part_total = inside[:, -1]
    suffix = part_total[:, None] - inside + forget_part
    return (query_gradient, key_gradient, value_gradient, grad_gate, suffix, part_total, back_decay, backward_matrix, back_vec)

def reference(block_input, queries, keys, values, in_gate, log_forget, grad_out):
    blocks = N_SP
    length = TOK_DEV
    query_blocks = queries.reshape(blocks, length, HEADS, DK)
    key_blocks = keys.reshape(blocks, length, HEADS, DK)
    value_blocks = values.reshape(blocks, length, HEADS, DV)
    grad_blocks = grad_out.reshape(blocks, length, HEADS, DV)
    gate_blocks = in_gate.reshape(HEADS, blocks, length).transpose(1, 0, 2)
    forget_blocks = log_forget.reshape(HEADS, blocks, length).transpose(1, 0, 2)

    def step_forward(running, inputs):
        summary = forward_summary(inputs[0], inputs[1], inputs[2], inputs[3])
        zero_head = jnp.zeros((HEADS,), jnp.float32)
        joined = join_forward((zero_head, running[0], running[1], running[2]), summary)
        return ((joined[1], joined[2], joined[3]), running)
    initial = (jnp.full((HEADS,), VERY_LOW, jnp.float32), jnp.zeros((HEADS, DK, DV), jnp.float32), jnp.zeros((HEADS, DK), jnp.float32))
    _, entered = lax.scan(step_forward, initial, (key_blocks, value_blocks, gate_blocks, forget_blocks))

    def step_back(back_carry, inputs):
        outgoing_matrix, outgoing_vector, tail_sum = back_carry
        results = local_pass(inputs[0], inputs[1], inputs[2], inputs[3], inputs[4], inputs[5], inputs[6], inputs[7], inputs[8], outgoing_matrix, outgoing_vector)
        query_gradient, key_gradient, value_gradient, grad_gate, suffix, part_total, back_decay, backward_matrix, back_vec = results
        keep_factor = jnp.exp(back_decay)
        new_carry = (backward_matrix + keep_factor[:, None, None] * outgoing_matrix, back_vec + keep_factor[:, None] * outgoing_vector, tail_sum + part_total)
        outputs = (query_gradient.astype(jnp.bfloat16), key_gradient.astype(jnp.bfloat16), value_gradient.astype(jnp.bfloat16), grad_gate, suffix + tail_sum[:, None])
        return (new_carry, outputs)
    back_start = (jnp.zeros((HEADS, DK, DV), jnp.float32), jnp.zeros((HEADS, DK), jnp.float32), jnp.zeros((HEADS,), jnp.float32))
    _, stacked = lax.scan(step_back, back_start, (query_blocks, key_blocks, value_blocks, grad_blocks, gate_blocks, forget_blocks, entered[0], entered[1], entered[2]), reverse=True)
    grad_queries = stacked[0].reshape(TOKENS, HEADS * DK)
    grad_keys = stacked[1].reshape(TOKENS, HEADS * DK)
    grad_values = stacked[2].reshape(TOKENS, HEADS * DV)
    grad_in_gate = stacked[3].transpose(1, 0, 2).reshape(HEADS, TOKENS)
    grad_log_forget = stacked[4].transpose(1, 0, 2).reshape(HEADS, TOKENS)
    grad_query_weight = jnp.dot(block_input.T, grad_queries, preferred_element_type=jnp.float32)
    return (grad_queries, grad_keys, grad_values, grad_in_gate, grad_log_forget, grad_query_weight)
```

```python
import functools

import jax
import jax.numpy as jnp
from jax import lax
from jax.experimental import pallas as pl
from jax.experimental.pallas import tpu as pltpu
from jax.sharding import PartitionSpec as P

VERY_LOW = -1e30
F32 = jnp.float32
BF16 = jnp.bfloat16
LANES = 128
SUBLANES = 8
UNROLLED = 32


def nn(a, b):
    return lax.dot_general(a, b, (((1,), (0,)), ((), ())), preferred_element_type=F32)


def nt(a, b):
    return lax.dot_general(a, b, (((1,), (1,)), ((), ())), preferred_element_type=F32)


def tn(a, b):
    return lax.dot_general(a, b, (((0,), (0,)), ((), ())), preferred_element_type=F32)


def thirds(a):
    high = a.astype(BF16)
    rest = a - high.astype(F32)
    middle = rest.astype(BF16)
    return high, middle, (rest - middle.astype(F32)).astype(BF16)


def loop(count, body, init):
    if count <= UNROLLED:
        for i in range(count):
            init = body(i, init)
        return init
    return lax.fori_loop(0, count, body, init)


def each(count, body):
    def one(i, carry):
        body(i)
        return carry

    loop(count, one, 0)


def side_tile(rows_of, size):
    row = lax.broadcasted_iota(jnp.int32, (LANES, size), 0)
    tile = jnp.zeros((LANES, size), F32)
    for i, value in enumerate(rows_of):
        tile = jnp.where(row == i, value, tile)
    return tile.T


def kernel(
    n, inner,
    b_ref, q_ref, k_ref, v_ref, gate_ref, forget_ref, g_ref,
    gq_ref, gk_ref, gv_ref, gg_ref, gf_ref, gw_ref,
    bt_ref, seg_ref, seg_in, ent_out, ent_in,
    back_ref, back_in, lea_out, lea_in,
    part_ref, plane_in, plane_out, line_in, tail_ref, tail_in,
    seg_s, seg_r, ent_s, ent_r, back_s, back_r, lea_s, lea_r,
    plane_s, plane_r, line_s, line_r, tail_s, tail_r,
):
    me = lax.axis_index("sp")
    outer = n // inner
    my_out, my_in = me // inner, lax.rem(me, inner)
    owners, rows = ent_in.shape[0], ent_in.shape[1]
    length, dk = q_ref.shape
    dv = v_ref.shape[1]
    share = gw_ref.shape[0]
    sigma = dk ** (-0.5)

    def copy(src, dst, send, recv, device):
        return pltpu.make_async_remote_copy(
            src_ref=src, dst_ref=dst, send_sem=send, recv_sem=recv,
            device_id={"sp": device}, device_id_type=pl.DeviceIdType.MESH,
        )

    barrier = pltpu.get_barrier_semaphore()

    def greet(i):
        @pl.when(i != me)
        def _():
            pl.semaphore_signal(
                barrier, inc=1, device_id={"sp": i}, device_id_type=pl.DeviceIdType.MESH
            )

    each(n, greet)

    at_row = lax.broadcasted_iota(jnp.int32, (length, length), 0)
    at_col = lax.broadcasted_iota(jnp.int32, (length, length), 1)

    def to_col(row):
        return jnp.sum(jnp.where(at_row == at_col, row, 0.0), axis=1, keepdims=True)

    def to_row(col):
        return jnp.sum(jnp.where(at_row == at_col, col, 0.0), axis=0, keepdims=True)

    queries, keys, values, grads = q_ref[...], k_ref[...], v_ref[...], g_ref[...]
    broad_query, broad_key = queries.astype(F32), keys.astype(F32)
    gate = gate_ref[...]
    forget = forget_ref[...]
    sum_col = jnp.sum(jnp.where(at_col <= at_row, forget, 0.0), axis=1, keepdims=True)
    sum_row = to_row(sum_col)
    total = sum_row[:, length - 1:]
    tail_row = total - sum_row + gate
    seg_max = jnp.max(tail_row, axis=1, keepdims=True)
    tail_col = to_col(tail_row)
    weighted = (broad_key * jnp.exp(tail_col - seg_max)).astype(BF16)
    seg_vec = sigma * jnp.sum(weighted.astype(F32), axis=0, keepdims=True)
    seg_ref[:, :dv] = sigma * tn(weighted, values)
    seg_ref[:, dv:] = side_tile((seg_vec, total, seg_max), dk)

    def give(buffer, arrived, send, recv):
        def one(i):
            @pl.when(i != me)
            def _():
                copy(
                    buffer.at[pl.ds(i * rows, rows)], arrived.at[me], send.at[i], recv.at[me], i
                ).start()

            @pl.when(i == me)
            def _():
                arrived[me] = buffer[pl.ds(i * rows, rows)]

        each(owners, one)

    def given(buffer, arrived, send, recv):
        def one(i):
            @pl.when(i != me)
            def _():
                copy(
                    buffer.at[pl.ds(i * rows, rows)], arrived.at[me], send.at[i], recv.at[me], i
                ).wait_send()

        each(owners, one)

    def await_part(buffer, arrived, send, recv, i):
        @pl.when(i != me)
        def _():
            copy(
                buffer.at[pl.ds(0, rows)], arrived.at[i], send.at[0], recv.at[i], i
            ).wait_recv()

    def hand(state_ref, arrived, send, recv, j):
        @pl.when(j != me)
        def _():
            copy(state_ref.at[j], arrived.at[me], send.at[j], recv.at[me], j).start()

        @pl.when(j == me)
        def _():
            arrived[me] = state_ref[j]

    def handed(state_ref, arrived, send, recv):
        def one(j):
            @pl.when(j != me)
            def _():
                copy(state_ref.at[j], arrived.at[me], send.at[j], recv.at[me], j).wait_send()

        each(n, one)

    def collect(state_ref, arrived, send, recv):
        def one(i):
            @pl.when(i != me)
            def _():
                copy(state_ref.at[0], arrived.at[i], send.at[0], recv.at[i], i).wait_recv()

        each(owners, one)
        return arrived[...].reshape(owners * rows, arrived.shape[2])

    pl.semaphore_wait(barrier, n - 1)
    give(seg_ref, seg_in, seg_s, seg_r)

    at_wide = lax.broadcasted_iota(jnp.int32, (rows, dv + LANES), 1)
    causal = at_col <= at_row
    log_intra = jnp.where(causal, sum_col - sum_row + gate, -jnp.inf)
    intra_max = jnp.max(log_intra, axis=1, keepdims=True)
    scores = sigma * nt(queries, keys)

    def owner_forward():
        def one(j, carry):
            run_max, state = carry
            ent_out[j] = jnp.where(at_wide == dv + 1, run_max, state)
            hand(ent_out, ent_in, ent_s, ent_r, j)
            await_part(seg_ref, seg_in, seg_s, seg_r, j)
            fresh = seg_in[j]
            decayed = fresh[:, dv + 1:dv + 2] + run_max
            top = fresh[:, dv + 2:dv + 3]
            new_max = jnp.maximum(decayed, top)
            state = jnp.exp(decayed - new_max) * state + jnp.exp(top - new_max) * fresh
            return new_max, state

        loop(n, one, (jnp.full((rows, 1), VERY_LOW, F32), jnp.zeros((rows, dv + LANES), F32)))

    if owners == n:
        owner_forward()
    else:
        pl.when(me < owners)(owner_forward)

    bt_ref[...] = b_ref[...].T

    entered = collect(ent_out, ent_in, ent_s, ent_r)
    enter_side = entered[:, dv:].T
    enter_vec = enter_side[0:1]
    enter_max = enter_side[1:2, 0:1]
    enter_low = entered[:, :dv].astype(BF16)

    log_inter = sum_col + enter_max
    row_max = jnp.maximum(log_inter, intra_max)
    inter = jnp.exp(log_inter - row_max)
    intra = jnp.exp(log_intra - row_max)
    weighted_scores = intra * scores
    score_low = weighted_scores.astype(BF16)
    numerator = inter * nn(queries, enter_low) + nn(score_low, values)
    denominator = inter * jnp.sum(broad_query * enter_vec, axis=1, keepdims=True) + jnp.sum(
        weighted_scores, axis=1, keepdims=True
    )
    floor_scale = jnp.sqrt(denominator * denominator + jnp.exp(-2.0 * row_max))
    broad_grad = grads.astype(F32)
    delta_low = (broad_grad / floor_scale).astype(BF16)
    epsilon = (
        -jnp.sum(broad_grad * numerator, axis=1, keepdims=True)
        * denominator
        / (floor_scale * floor_scale * floor_scale)
    )
    leave_max = jnp.maximum(total + enter_max, seg_max)
    decay = total + enter_max - leave_max
    inter_query = inter * broad_query
    back_ref[:, :dv] = tn(inter_query.astype(BF16), delta_low)
    back_vec = jnp.sum(epsilon * inter_query, axis=0, keepdims=True)
    back_ref[:, dv:] = side_tile((back_vec, decay), dk)
    errors = nt(delta_low, values) + epsilon
    back_low = (intra * errors).astype(BF16)
    give(back_ref, back_in, back_s, back_r)

    grad_query = sigma * nn(back_low, keys) + inter * (
        nt(delta_low, enter_low) + epsilon * enter_vec
    )
    query_low = grad_query.astype(BF16)
    gq_ref[...] = query_low
    row_part = jnp.sum(broad_query * grad_query, axis=1, keepdims=True)
    part_ref[...] = nn(bt_ref[...], query_low)

    order = sorted(range(1, outer), key=lambda k: abs(2 * k - outer)) + [0]

    def plane_copy(far, p):
        return copy(
            part_ref.at[pl.ds((far * inner + p) * share, share)], plane_in.at[far, my_in],
            plane_s.at[far, p], plane_r.at[far, my_in], my_out * inner + p,
        )

    def plane_arrival(far, p):
        return copy(
            part_ref.at[pl.ds(0, share)], plane_in.at[far, p],
            plane_s.at[far, p], plane_r.at[far, p], my_out * inner + p,
        )

    for k in order:
        far = lax.rem(my_out + k, outer)

        for step in range(1, inner):
            plane_copy(far, lax.rem(my_in + step, inner)).start()

    key_intra = sigma * tn(back_low, queries)
    value_intra = tn(score_low, delta_low)
    key_decay = sigma * jnp.exp(tail_col - leave_max)

    def owner_back():
        def one(lap, state):
            j = n - 1 - lap
            lea_out[j] = state
            hand(lea_out, lea_in, lea_s, lea_r, j)
            await_part(back_ref, back_in, back_s, back_r, j)
            fresh = back_in[j]
            return fresh + jnp.exp(fresh[:, dv + 1:dv + 2]) * state

        loop(n, one, jnp.zeros((rows, dv + LANES), F32))

    if owners == n:
        owner_back()
    else:
        pl.when(me < owners)(owner_back)

    def line_copy(far):
        return copy(
            plane_out.at[far], line_in.at[my_out], line_s.at[far], line_r.at[my_out],
            far * inner + my_in,
        )

    for k in order:
        far = lax.rem(my_out + k, outer)
        joined = part_ref[pl.ds((far * inner + my_in) * share, share)]
        for step in range(1, inner):
            source = lax.rem(my_in + step, inner)
            plane_arrival(far, source).wait_recv()
            joined = joined + plane_in[far, source]
        plane_out[far] = joined
        if k:
            line_copy(far).start()

    left = collect(lea_out, lea_in, lea_s, lea_r)
    leave_vec = left[:, dv:].T[0:1]
    pieces = thirds(left[:, :dv])
    from_values = nt(values, pieces[2]) + nt(values, pieces[1]) + nt(values, pieces[0])
    from_keys = nn(keys, pieces[2]) + nn(keys, pieces[1]) + nn(keys, pieces[0])
    grad_key = key_intra + key_decay * (from_values + leave_vec)
    gate_col = jnp.sum(broad_key * grad_key, axis=1, keepdims=True)
    forget_part = row_part - gate_col
    part_total = jnp.sum(forget_part, axis=0, keepdims=True)
    tail_ref[...] = jnp.broadcast_to(part_total, tail_ref.shape)
    gk_ref[...] = grad_key.astype(BF16)
    gg_ref[...] = to_row(gate_col)
    suffix = jnp.sum(jnp.where(at_row >= at_col, forget_part, 0.0), axis=0, keepdims=True)

    def tail_copy(i):
        return copy(tail_ref, tail_in.at[me], tail_s.at[i], tail_r.at[me], i)

    def tell(i):
        @pl.when(i < me)
        def _():
            tail_copy(i).start()

    each(n, tell)
    gv_ref[...] = (value_intra + key_decay * from_keys).astype(BF16)

    whole = plane_out[my_out]
    for k in order[:-1]:
        far = lax.rem(my_out + k, outer)
        copy(
            plane_out.at[far], line_in.at[far], line_s.at[far], line_r.at[far],
            far * inner + my_in,
        ).wait_recv()
        whole = whole + line_in[far]
    gw_ref[...] = whole

    tail_in[me] = jnp.zeros(tail_ref.shape, F32)

    def hear(i):
        @pl.when(i > me)
        def _():
            copy(tail_ref, tail_in.at[i], tail_s.at[i], tail_r.at[i], i).wait_recv()

        @pl.when(i < me)
        def _():
            tail_in[i] = jnp.zeros(tail_ref.shape, F32)

    each(n, hear)
    later = jnp.sum(tail_in[...], axis=0)
    gf_ref[...] = suffix + later[0:1, 0:1]

    given(seg_ref, seg_in, seg_s, seg_r)
    given(back_ref, back_in, back_s, back_r)

    def owner_end():
        handed(ent_out, ent_in, ent_s, ent_r)
        handed(lea_out, lea_in, lea_s, lea_r)

    if owners == n:
        owner_end()
    else:
        pl.when(me < owners)(owner_end)
    for k in order:
        far = lax.rem(my_out + k, outer)
        for step in range(1, inner):
            plane_copy(far, lax.rem(my_in + step, inner)).wait_send()
        if k:
            line_copy(far).wait_send()

    def told(i):
        @pl.when(i < me)
        def _():
            tail_copy(i).wait_send()

    each(n, told)


def on_device(n, block_input, queries, keys, values, in_gate, log_forget, grad_out):
    length, dk = queries.shape
    dv = values.shape[1]
    width = block_input.shape[1]
    rows = max(SUBLANES, dk // n)
    owners = dk // rows
    share = width // n
    inner = max(d for d in range(1, n + 1) if n % d == 0 and d * d <= n)
    outer = n // inner
    wide = dv + LANES
    tile = (SUBLANES, LANES)
    vmem = pl.BlockSpec(memory_space=pltpu.VMEM)
    dma = pltpu.SemaphoreType.DMA
    return pl.pallas_call(
        functools.partial(kernel, n, inner),
        out_shape=(
            jax.ShapeDtypeStruct((length, dk), BF16),
            jax.ShapeDtypeStruct((length, dk), BF16),
            jax.ShapeDtypeStruct((length, dv), BF16),
            jax.ShapeDtypeStruct((1, length), F32),
            jax.ShapeDtypeStruct((1, length), F32),
            jax.ShapeDtypeStruct((share, dk), F32),
        ),
        in_specs=[vmem] * 7,
        out_specs=(vmem,) * 6,
        scratch_shapes=[
            pltpu.VMEM((width, length), BF16),
            pltpu.VMEM((dk, wide), F32),
            pltpu.VMEM((n, rows, wide), F32),
            pltpu.VMEM((n, rows, wide), F32),
            pltpu.VMEM((owners, rows, wide), F32),
            pltpu.VMEM((dk, wide), F32),
            pltpu.VMEM((n, rows, wide), F32),
            pltpu.VMEM((n, rows, wide), F32),
            pltpu.VMEM((owners, rows, wide), F32),
            pltpu.VMEM((width, dk), F32),
            pltpu.VMEM((outer, inner, share, dk), F32),
            pltpu.VMEM((outer, share, dk), F32),
            pltpu.VMEM((outer, share, dk), F32),
            pltpu.VMEM(tile, F32),
            pltpu.VMEM((n,) + tile, F32),
            dma((owners,)), dma((n,)), dma((n,)), dma((owners,)),
            dma((owners,)), dma((n,)), dma((n,)), dma((owners,)),
            dma((outer, inner)), dma((outer, inner)), dma((outer,)), dma((outer,)),
            dma((n,)), dma((n,)),
        ],
        compiler_params=pltpu.CompilerParams(collective_id=0, has_side_effects=True),
    )(block_input, queries, keys, values, in_gate, log_forget, grad_out)


def solution(mesh):
    seq, both, gates = P("sp", None), P("sp", "tp"), P("tp", "sp")
    return jax.shard_map(
        functools.partial(on_device, mesh.shape["sp"]),
        mesh=mesh,
        in_specs=(seq, both, both, both, gates, gates, both),
        out_specs=(both, both, both, gates, gates, both),
        check_vma=False,
    )
```

```python
import functools

import jax
import jax.numpy as jnp
from jax import lax
from jax.experimental import pallas as pl
from jax.experimental.pallas import tpu as pltpu
from jax.sharding import PartitionSpec as P

VERY_LOW = -1e30
F32 = jnp.float32
BF16 = jnp.bfloat16
LANES = 128
SUBLANES = 8
UNROLLED = 32


def nn(a, b):
    return lax.dot_general(a, b, (((1,), (0,)), ((), ())), preferred_element_type=F32)


def nt(a, b):
    return lax.dot_general(a, b, (((1,), (1,)), ((), ())), preferred_element_type=F32)


def tn(a, b):
    return lax.dot_general(a, b, (((0,), (0,)), ((), ())), preferred_element_type=F32)


def thirds(a):
    high = a.astype(BF16)
    rest = a - high.astype(F32)
    middle = rest.astype(BF16)
    return high, middle, (rest - middle.astype(F32)).astype(BF16)


def loop(count, body, init):
    if count <= UNROLLED:
        for i in range(count):
            init = body(i, init)
        return init
    return lax.fori_loop(0, count, body, init)


def each(count, body):
    def one(i, carry):
        body(i)
        return carry

    loop(count, one, 0)


def side_tile(rows_of, size):
    row = lax.broadcasted_iota(jnp.int32, (LANES, size), 0)
    tile = jnp.zeros((LANES, size), F32)
    for i, value in enumerate(rows_of):
        tile = jnp.where(row == i, value, tile)
    return tile.T


def kernel(
    n, inner,
    b_ref, q_ref, k_ref, v_ref, gate_ref, forget_ref, g_ref,
    gq_ref, gk_ref, gv_ref, gg_ref, gf_ref, gw_ref,
    bt_ref, seg_ref, seg_in, ent_out, ent_in,
    back_ref, back_in, lea_out, lea_in,
    part_ref, plane_in, plane_out, line_in,
    seg_s, seg_r, ent_s, ent_r, back_s, back_r, lea_s, lea_r,
    plane_s, plane_r, line_s, line_r, wide_ref, wide_s,
):
    me = lax.axis_index("sp")
    outer = n // inner
    my_out, my_in = me // inner, lax.rem(me, inner)
    owners, rows = ent_in.shape[0], ent_in.shape[1]
    length, dk = q_ref.shape
    dv = v_ref.shape[1]
    share = gw_ref.shape[0]
    sigma = dk ** (-0.5)

    def copy(src, dst, send, recv, device):
        return pltpu.make_async_remote_copy(
            src_ref=src, dst_ref=dst, send_sem=send, recv_sem=recv,
            device_id={"sp": device}, device_id_type=pl.DeviceIdType.MESH,
        )

    barrier = pltpu.get_barrier_semaphore()

    def others(body):
        def one(k):
            far = (k + 1) // 2
            body(lax.rem(me + (n // 2 + (far if k % 2 else -far) if n <= UNROLLED else k + 1) + n, n))

        each(n - 1, one)

    def greet(i):
        pl.semaphore_signal(
            barrier, inc=1, device_id={"sp": i}, device_id_type=pl.DeviceIdType.MESH
        )

    others(greet)
    fetch = pltpu.make_async_copy(b_ref, wide_ref, wide_s)
    fetch.start()

    def other_owners(body):
        def one(i):
            if owners == n:
                body(i)
            else:
                pl.when(i < owners)(lambda: body(i))

        others(one)

    def as_owner(body):
        if owners == n:
            body()
        else:
            pl.when(me < owners)(body)

    at_row = lax.broadcasted_iota(jnp.int32, (length, length), 0)
    at_col = lax.broadcasted_iota(jnp.int32, (length, length), 1)

    def to_col(row):
        return jnp.sum(jnp.where(at_row == at_col, row, 0.0), axis=1, keepdims=True)

    def to_row(col):
        return jnp.sum(jnp.where(at_row == at_col, col, 0.0), axis=0, keepdims=True)

    queries, keys, values, grads = q_ref[...], k_ref[...], v_ref[...], g_ref[...]
    broad_query, broad_key = queries.astype(F32), keys.astype(F32)
    gate = gate_ref[...]
    forget = forget_ref[...]
    sum_col = jnp.sum(jnp.where(at_col <= at_row, forget, 0.0), axis=1, keepdims=True)
    sum_row = to_row(sum_col)
    total = sum_row[:, length - 1:]
    tail_row = total - sum_row + gate
    seg_max = jnp.max(tail_row, axis=1, keepdims=True)
    tail_col = to_col(tail_row)
    weighted = (broad_key * jnp.exp(tail_col - seg_max)).astype(BF16)
    seg_vec = sigma * jnp.sum(weighted.astype(F32), axis=0, keepdims=True)
    seg_ref[:, :dv] = sigma * tn(weighted, values)
    seg_ref[:, dv:] = side_tile((seg_vec, total, seg_max), dk)

    def give_copy(buffer, arrived, send, recv, i):
        start = pl.multiple_of(i * rows, rows)
        return copy(buffer.at[pl.ds(start, rows)], arrived.at[me], send.at[i], recv.at[me], i)

    def give(buffer, arrived, send, recv):
        other_owners(lambda i: give_copy(buffer, arrived, send, recv, i).start())

        def own():
            arrived[me] = buffer[pl.ds(pl.multiple_of(me * rows, rows), rows)]

        as_owner(own)

    def given(buffer, arrived, send, recv):
        other_owners(lambda i: give_copy(buffer, arrived, send, recv, i).wait_send())

    def await_parts(buffer, arrived, send, recv):
        others(
            lambda i: copy(
                buffer.at[pl.ds(0, rows)], arrived.at[i], send.at[0], recv.at[i], i
            ).wait_recv()
        )

    def hand(state_ref, arrived, send, recv):
        others(
            lambda j: copy(
                state_ref.at[j], arrived.at[me], send.at[j], recv.at[me], j
            ).start()
        )
        arrived[me] = state_ref[me]

    def handed(state_ref, arrived, send, recv):
        others(
            lambda j: copy(
                state_ref.at[j], arrived.at[me], send.at[j], recv.at[me], j
            ).wait_send()
        )

    def collect(state_ref, arrived, send, recv):
        other_owners(
            lambda i: copy(
                state_ref.at[0], arrived.at[i], send.at[0], recv.at[i], i
            ).wait_recv()
        )
        return arrived[...].reshape(owners * rows, arrived.shape[2])

    pl.semaphore_wait(barrier, n - 1)
    give(seg_ref, seg_in, seg_s, seg_r)

    at_wide = lax.broadcasted_iota(jnp.int32, (rows, dv + LANES), 1)
    causal = at_col <= at_row
    log_intra = jnp.where(causal, sum_col - sum_row + gate, -jnp.inf)
    intra_max = jnp.max(log_intra, axis=1, keepdims=True)
    scores = sigma * nt(queries, keys)

    def owner_forward():
        await_parts(seg_ref, seg_in, seg_s, seg_r)

        def one(j, carry):
            run_max, state = carry
            ent_out[j] = jnp.where(at_wide == dv + 1, run_max, state)
            fresh = seg_in[j]
            decayed = fresh[:, dv + 1:dv + 2] + run_max
            top = fresh[:, dv + 2:dv + 3]
            new_max = jnp.maximum(decayed, top)
            state = jnp.exp(decayed - new_max) * state + jnp.exp(top - new_max) * fresh
            return new_max, state

        loop(n, one, (jnp.full((rows, 1), VERY_LOW, F32), jnp.zeros((rows, dv + LANES), F32)))
        hand(ent_out, ent_in, ent_s, ent_r)

    as_owner(owner_forward)
    fetch.wait()
    bt_ref[...] = wide_ref[...].T

    entered = collect(ent_out, ent_in, ent_s, ent_r)
    enter_side = entered[:, dv:].T
    enter_vec = enter_side[0:1]
    enter_max = enter_side[1:2, 0:1]
    enter_low = entered[:, :dv].astype(BF16)

    log_inter = sum_col + enter_max
    row_max = jnp.maximum(log_inter, intra_max)
    inter = jnp.exp(log_inter - row_max)
    intra = jnp.exp(log_intra - row_max)
    weighted_scores = intra * scores
    score_low = weighted_scores.astype(BF16)
    numerator = inter * nn(queries, enter_low) + nn(score_low, values)
    denominator = inter * jnp.sum(broad_query * enter_vec, axis=1, keepdims=True) + jnp.sum(
        weighted_scores, axis=1, keepdims=True
    )
    floor_scale = jnp.sqrt(denominator * denominator + jnp.exp(-2.0 * row_max))
    broad_grad = grads.astype(F32)
    delta_low = (broad_grad / floor_scale).astype(BF16)
    epsilon = (
        -jnp.sum(broad_grad * numerator, axis=1, keepdims=True)
        * denominator
        / (floor_scale * floor_scale * floor_scale)
    )
    leave_max = jnp.maximum(total + enter_max, seg_max)
    decay = total + enter_max - leave_max
    leaving = jnp.exp(decay) * entered + jnp.exp(seg_max - leave_max) * seg_ref[...]
    inter_query = inter * broad_query
    back_ref[:, :dv] = tn(inter_query.astype(BF16), delta_low)
    back_vec = jnp.sum(epsilon * inter_query, axis=0, keepdims=True)
    back_ref[:, dv:] = side_tile((back_vec, decay), dk)
    errors = nt(delta_low, values) + epsilon
    back_low = (intra * errors).astype(BF16)
    give(back_ref, back_in, back_s, back_r)

    grad_query = sigma * nn(back_low, keys) + inter * (
        nt(delta_low, enter_low) + epsilon * enter_vec
    )
    query_low = grad_query.astype(BF16)
    gq_ref[...] = query_low
    row_part = jnp.sum(broad_query * grad_query, axis=1, keepdims=True)
    part_ref[...] = nn(bt_ref[...], query_low)

    order = sorted(range(1, outer), key=lambda k: abs(2 * k - outer)) + [0]

    def plane_copy(far, p):
        return copy(
            part_ref.at[pl.ds((far * inner + p) * share, share)], plane_in.at[far, my_in],
            plane_s.at[far, p], plane_r.at[far, my_in], my_out * inner + p,
        )

    def plane_arrival(far, p):
        return copy(
            part_ref.at[pl.ds(0, share)], plane_in.at[far, p],
            plane_s.at[far, p], plane_r.at[far, p], my_out * inner + p,
        )

    def plane_start(turns):
        for k in turns:
            for step in range(1, inner):
                plane_copy(lax.rem(my_out + k, outer), lax.rem(my_in + step, inner)).start()

    plane_start(order)

    key_intra = sigma * tn(back_low, queries)
    value_intra = tn(score_low, delta_low)
    key_decay = sigma * jnp.exp(tail_col - leave_max)

    def owner_back():
        await_parts(back_ref, back_in, back_s, back_r)

        def one(lap, state):
            j = n - 1 - lap
            lea_out[j] = state
            fresh = back_in[j]
            return fresh + jnp.exp(fresh[:, dv + 1:dv + 2]) * state

        loop(n, one, jnp.zeros((rows, dv + LANES), F32))
        hand(lea_out, lea_in, lea_s, lea_r)

    as_owner(owner_back)

    def line_copy(far):
        return copy(
            plane_out.at[far], line_in.at[my_out], line_s.at[far], line_r.at[my_out],
            far * inner + my_in,
        )

    for k in order:
        far = lax.rem(my_out + k, outer)
        joined = part_ref[pl.ds((far * inner + my_in) * share, share)]
        for step in range(1, inner):
            source = lax.rem(my_in + step, inner)
            plane_arrival(far, source).wait_recv()
            joined = joined + plane_in[far, source]
        plane_out[far] = joined
        if k:
            line_copy(far).start()

    left = collect(lea_out, lea_in, lea_s, lea_r)
    leave_vec = left[:, dv:].T[0:1]
    pieces = thirds(left[:, :dv])
    from_values = nt(values, pieces[2]) + nt(values, pieces[1]) + nt(values, pieces[0])
    from_keys = nn(keys, pieces[2]) + nn(keys, pieces[1]) + nn(keys, pieces[0])
    grad_key = key_intra + key_decay * (from_values + leave_vec)
    gate_col = jnp.sum(broad_key * grad_key, axis=1, keepdims=True)
    forget_part = row_part - gate_col
    gk_ref[...] = grad_key.astype(BF16)
    gg_ref[...] = to_row(gate_col)
    suffix = jnp.sum(jnp.where(at_row >= at_col, forget_part, 0.0), axis=0, keepdims=True)

    at_side = lax.broadcasted_iota(jnp.int32, left.shape, 1)
    pairing = jnp.where(at_side <= dv, left * leaving, 0.0)
    later = jnp.sum(jnp.sum(pairing, axis=1, keepdims=True), axis=0, keepdims=True)
    gf_ref[...] = suffix + later
    gv_ref[...] = (value_intra + key_decay * from_keys).astype(BF16)

    whole = plane_out[my_out]
    for k in order[:-1]:
        far = lax.rem(my_out + k, outer)
        copy(
            plane_out.at[far], line_in.at[far], line_s.at[far], line_r.at[far],
            far * inner + my_in,
        ).wait_recv()
        whole = whole + line_in[far]
    gw_ref[...] = whole

    given(seg_ref, seg_in, seg_s, seg_r)
    given(back_ref, back_in, back_s, back_r)

    def owner_end():
        handed(ent_out, ent_in, ent_s, ent_r)
        handed(lea_out, lea_in, lea_s, lea_r)

    as_owner(owner_end)
    for k in order:
        far = lax.rem(my_out + k, outer)
        for step in range(1, inner):
            plane_copy(far, lax.rem(my_in + step, inner)).wait_send()
        if k:
            line_copy(far).wait_send()


def settle(*refs):
    half = len(refs) // 2
    sems = refs[-1]
    moves = [
        pltpu.make_async_copy(refs[i], refs[half + i], sems.at[i]) for i in range(half)
    ]
    for move in moves:
        move.start()
    for move in moves:
        move.wait()


def on_device(n, block_input, queries, keys, values, in_gate, log_forget, grad_out):
    length, dk = queries.shape
    dv = values.shape[1]
    width = block_input.shape[1]
    rows = max(SUBLANES, dk // n)
    owners = dk // rows
    share = width // n
    inner = max(d for d in range(1, n + 1) if n % d == 0 and d * d <= n)
    outer = n // inner
    wide = dv + LANES
    vmem = pl.BlockSpec(memory_space=pltpu.VMEM)
    dma = pltpu.SemaphoreType.DMA
    results = (
        ((length, dk), BF16), ((length, dk), BF16), ((length, dv), BF16),
        ((1, length), F32), ((1, length), F32), ((share, dk), F32),
    )
    held = pl.pallas_call(
        functools.partial(kernel, n, inner),
        out_shape=tuple(pltpu.VMEM(*r) for r in results),
        in_specs=[pl.BlockSpec(memory_space=pl.ANY)] + [vmem] * 6,
        out_specs=(vmem,) * 6,
        scratch_shapes=[
            pltpu.VMEM((width, length), BF16),
            pltpu.VMEM((dk, wide), F32),
            pltpu.VMEM((n, rows, wide), F32),
            pltpu.VMEM((n, rows, wide), F32),
            pltpu.VMEM((owners, rows, wide), F32),
            pltpu.VMEM((dk, wide), F32),
            pltpu.VMEM((n, rows, wide), F32),
            pltpu.VMEM((n, rows, wide), F32),
            pltpu.VMEM((owners, rows, wide), F32),
            pltpu.VMEM((width, dk), F32),
            pltpu.VMEM((outer, inner, share, dk), F32),
            pltpu.VMEM((outer, share, dk), F32),
            pltpu.VMEM((outer, share, dk), F32),
            dma((owners,)), dma((n,)), dma((n,)), dma((owners,)),
            dma((owners,)), dma((n,)), dma((n,)), dma((owners,)),
            dma((outer, inner)), dma((outer, inner)), dma((outer,)), dma((outer,)),
            pltpu.VMEM((length, width), BF16), dma,
        ],
        compiler_params=pltpu.CompilerParams(collective_id=0, has_side_effects=True),
    )(block_input, queries, keys, values, in_gate, log_forget, grad_out)
    held = [pltpu.with_memory_space_constraint(h, pltpu.VMEM) for h in held]
    return pl.pallas_call(
        settle,
        out_shape=tuple(jax.ShapeDtypeStruct(*r) for r in results),
        in_specs=[vmem] * 6,
        out_specs=(pl.BlockSpec(memory_space=pl.ANY),) * 6,
        scratch_shapes=[dma((6,))],
    )(*held)


def solution(mesh):
    seq, both, gates = P("sp", None), P("sp", "tp"), P("tp", "sp")
    return jax.shard_map(
        functools.partial(on_device, mesh.shape["sp"]),
        mesh=mesh,
        in_specs=(seq, both, both, both, gates, gates, both),
        out_specs=(both, both, both, gates, gates, both),
        check_vma=False,
    )
```
